128 devices in a mesh: sp: 32 (over z, y, core), tp: 4 (over x).
Axes of the slice: x: 4, y: 4, z: 4, core: 2. Of those that a mesh axis runs over, the one named last changes fastest.
Arguments:
- residual: bfloat16 [8192, 2048], P(('sp', 'tp')), may hold values from -6 to 6
- receptance: bfloat16 [8192, 768], P('sp', 'tp'), may hold values from -6 to 6
- key_matrix: bfloat16 [8192, 768], P('sp', 'tp'), may hold values from -6 to 6
- values: bfloat16 [8192, 768], P('sp', 'tp'), may hold values from -6 to 6
- decay_dependent_logit: bfloat16 [8192, 768], P('sp', 'tp'), may hold values from -3.5 to 3.5
- decay_channel_offset: float32 [768], P('tp'), may hold values from -12.5 to -2.4
- extra_log_decay: float32 [8192, 768], P('sp', 'tp'), may hold values from -2.1 to 0
- removal_dependent_logit: bfloat16 [8192, 768], P('sp', 'tp'), may hold values from -4 to 4
- removal_channel_offset: float32 [768], P('tp'), may hold values from -8.1 to 0.5
- head_norm_gain: float32 [768], P('tp'), may hold values from 0.1 to 1.9
- output_matrix: bfloat16 [768, 2048], replicated, may hold values from -0.21875 to 0.21875
- expert_norm_gain: float32 [2048], replicated, may hold values from 0.1 to 1.9
- token_expert_index: int32 [8192, 2], P(('sp', 'tp')), may hold values from 0 to 31, all different within a row; in each aligned block of 64 rows (0 to 63, 64 to 127, ...) at most 8 rows name the same one
- token_expert_weight: float32 [8192, 2], P(('sp', 'tp')), may hold values from 0.2 to 1
- expert_gate_weight: bfloat16 [32, 2048, 3584], P('sp', None, 'tp'), may hold values from -0.125 to 0.125
- expert_up_weight: bfloat16 [32, 2048, 3584], P('sp', None, 'tp'), may hold values from -0.125 to 0.125
- expert_down_weight: bfloat16 [32, 3584, 2048], P('sp', 'tp'), may hold values from -0.09375 to 0.09375
Outputs:
- output: bfloat16 [8192, 2048], P(('sp', 'tp'))
The draws below stay inside these ranges and needn't reach their ends.
Inputs may be any that keep to these rules, and one draw needn't show every extreme that they name: `token_expert_index`: each row names 2 different experts. In each aligned block of 64 rows no expert is named by more than 8 rows, and in every draw some expert is named by exactly 8 rows of some block.
All inputs are finite; a program needn't handle non-finite values.
Results may differ from the reference program's by a relative error of at most 0.015.
Values may be sent and summed in bfloat16 or wider, within the bound.
A program may use at most 128 MiB of HBM per device.

```python
import math
import jax
import jax.numpy as jnp
import numpy as np
from jax import lax

D = 2048
HEADS = 12
HEAD = 64
RW = 768
FF = 3584
TOP = 2
TOK_DEV = 256
TOKENS = 8192
ROWS_DEV = 64
EXPERTS = 32
CAP = 8
N_SP = 32
N_TP = 4


def head_speed(key, share):
    pick = jax.random.uniform(jax.random.fold_in(key, 5), (HEADS,), jnp.float32)
    return jnp.repeat((pick < share).astype(jnp.float32), HEAD)


def draw_decay_channel_offset(key, part):
    fast = head_speed(key, 0.5)
    jitter = jax.random.uniform(jax.random.fold_in(key, 6), (HEADS * HEAD,), jnp.float32, -0.5, 0.5)
    slow_level = -jnp.log(jnp.float32(TOKENS)) - 1.5
    return fast * -2.9 + (1.0 - fast) * slow_level + jitter


def draw_removal_channel_offset(key, part):
    fast = head_speed(key, 0.5)
    jitter = jax.random.uniform(jax.random.fold_in(key, 8), (HEADS * HEAD,), jnp.float32, -0.5, 0.5)
    slow_level = jnp.log(jnp.float32(HEAD) / jnp.float32(TOKENS)) - 2.0
    return (1.0 - fast) * slow_level + jitter


def draw_decay_dependent_logit(key, part):
    noise = jnp.clip(jax.random.normal(jax.random.fold_in(key, 1), (TOKENS, HEADS * HEAD), jnp.float32), -4.0, 4.0) * 0.7
    offset = jax.random.uniform(jax.random.fold_in(key, 2), (TOKENS // TOK_DEV, 1, 1), jnp.float32, -0.7, 0.7)
    shaped = noise.reshape(TOKENS // TOK_DEV, TOK_DEV, HEADS * HEAD) + offset
    return shaped.reshape(TOKENS, HEADS * HEAD).astype(jnp.bfloat16)


def draw_extra_log_decay(key, part):
    spots = jax.random.randint(jax.random.fold_in(key, 3), (3,), 0, TOKENS)
    kept = jax.random.uniform(jax.random.fold_in(key, 4), (3, HEADS * HEAD), jnp.float32, 0.5, 0.8)
    hits = (jnp.arange(TOKENS)[:, None] == spots[None, :]).astype(jnp.float32)
    return jnp.dot(hits, jnp.log(kept), precision=lax.Precision.HIGHEST)


def level_of(own_key, dims, pieces, low, largest):
    level, own = 1.0, jax.random.fold_in(own_key, 6)
    for axis_at, blocks in pieces:
        steps = jnp.exp(jax.random.uniform(jax.random.fold_in(own, axis_at), (blocks,), jnp.float32, low / len(pieces), largest / len(pieces)))
        level = level * jnp.repeat(steps, dims[axis_at] // blocks).reshape([-1 if axis == axis_at else 1 for axis in range(len(dims))])
    return level


def routed_block(key, own, number, rows, amount, top, bound, slope):
    ranking = jax.random.permutation(key, amount)
    packed, ordinary = portions_of(amount, rows * top, bound, slope, True), portions_of(amount, rows * top, bound, slope, False)
    places = jnp.arange(amount)

    def named(lengths, offset_by):
        used = int((lengths > 0).sum())
        fixed = max(1, used // 4)
        shifted = fixed + (places - fixed + offset_by * (used - fixed)) % max(1, amount - fixed)
        return jnp.zeros((amount,), jnp.int32).at[ranking[jnp.where(places < fixed, places, shifted)]].set(jnp.asarray(lengths, jnp.int32))

    lengths = jnp.where(number % 4 == 0, named(packed, number // 4), named(ordinary, number - number // 4 - 1))
    mixed = jax.random.permutation(jax.random.fold_in(own, 3), amount)
    source_of, receiver = mixed[0:amount // 2 * 2:2], mixed[1:amount // 2 * 2:2]
    margin = jnp.minimum(lengths[source_of] - 1, bound - lengths[receiver]) // 2
    margin = jnp.where((source_of == ranking[0]) | (receiver == ranking[0]) | (lengths[receiver] == 0), 0, jnp.maximum(margin, 0))
    shifted = jax.random.randint(jax.random.fold_in(own, 4), (amount // 2,), 0, 1 << 20) % (margin + 1)
    lengths = lengths.at[source_of].add(-shifted).at[receiver].add(shifted)
    labels = jnp.searchsorted(jnp.cumsum(lengths), jnp.arange(rows * top), side="right").astype(jnp.int32)
    grid = labels.reshape(top, rows).T
    grid = grid[jax.random.permutation(jax.random.fold_in(own, 1), rows)]
    offset_by = jax.random.randint(jax.random.fold_in(own, 2), (rows, 1), 0, top)
    return jnp.take_along_axis(grid, (jnp.arange(top)[None, :] + offset_by) % top, axis=1)


def portions_of(count, total, bound, slope, full):
    portions = [(1 << 20) // math.isqrt(rank ** slope) + 1 for rank in range(1, count + 1)]
    largest = bound if full else min(bound, max(-(-total // count), total * portions[0] // sum(portions)))
    least = 1 if total - largest >= count - 1 else 0
    given, surplus = [largest] + [least] * (count - 1), total - largest - least * (count - 1)
    while surplus > 0:
        free = [i for i in range(1, count) if given[i] < largest] or [i for i in range(1, count) if given[i] < bound]
        pool, left = sum([portions[i] for i in free]), surplus
        for i in free:
            extra = min(bound - given[i], max(1, left * portions[i] // pool), surplus)
            given[i] = given[i] + extra
            surplus = surplus - extra
    return np.array(given)


def centred(stream_key, shape, scale, bound, pieces=(), kind=jnp.bfloat16):
    result = scale * jax.random.normal(stream_key, shape, jnp.float32)
    if pieces:
        result = result * level_of(stream_key, shape, pieces, -0.22, 0.18)
    return jnp.clip(result, -bound, bound).astype(kind)


def setup_inputs(seed: int = 0) -> dict:
    key_of = jax.random.split(jax.random.key(seed), 18)
    residual = centred(key_of[0], (TOKENS, D), 1.0, 6.0, ((0, 128),))
    receptance = centred(key_of[1], (TOKENS, RW), 1.0, 6.0, ((0, 32), (1, 4)))
    key_matrix = centred(key_of[2], (TOKENS, RW), 1.0, 6.0, ((0, 32), (1, 4)))
    values = centred(key_of[3], (TOKENS, RW), 1.0, 6.0, ((0, 32), (1, 4)))
    decay_dependent_logit = draw_decay_dependent_logit(jax.random.fold_in(key_of[17], 71), 0)
    decay_channel_offset = draw_decay_channel_offset(jax.random.fold_in(key_of[17], 71), 0)
    extra_log_decay = draw_extra_log_decay(jax.random.fold_in(key_of[17], 71), 0)
    removal_dependent_logit = centred(key_of[7], (TOKENS, RW), 1.0, 4.0, ((0, 32), (1, 4)))
    removal_channel_offset = draw_removal_channel_offset(jax.random.fold_in(key_of[17], 71), 0)
    head_norm_gain = jnp.clip(1.0 + 0.18 * jax.random.normal(key_of[9], (RW,), jnp.float32), 0.1, 1.9)
    output_matrix = centred(key_of[10], (RW, D), RW ** -0.5, 0.21875)
    expert_norm_gain = jnp.clip(1.0 + 0.18 * jax.random.normal(key_of[11], (D,), jnp.float32), 0.1, 1.9)
    token_expert_index_keys = jax.random.split(jax.random.fold_in(key_of[12], 1), TOKENS // ROWS_DEV)
    token_expert_index_turns = jax.random.permutation(jax.random.fold_in(key_of[12], 3), TOKENS // ROWS_DEV)
    token_expert_index = jax.vmap(lambda own, number: routed_block(jax.random.fold_in(key_of[12], 2), own, number, ROWS_DEV, EXPERTS, TOP, CAP, 2))(token_expert_index_keys, token_expert_index_turns).reshape((TOKENS, TOP))
    token_expert_weight = jnp.clip(0.2 + 0.8 * jax.random.uniform(key_of[13], (TOKENS, TOP), jnp.float32) ** level_of(key_of[13], (TOKENS, TOP), ((0, 128),), -0.2, 0.2), 0.2, 1.0)
    expert_gate_weight = centred(key_of[14], (EXPERTS, D, FF), D ** -0.5, 0.125, ((0, 32), (2, 4)))
    expert_up_weight = centred(key_of[15], (EXPERTS, D, FF), D ** -0.5, 0.125, ((0, 32), (2, 4)))
    expert_down_weight = centred(key_of[16], (EXPERTS, FF, D), FF ** -0.5, 0.09375, ((0, 32), (1, 4)))
    return {"residual": residual, "receptance": receptance, "key_matrix": key_matrix, "values": values, "decay_dependent_logit": decay_dependent_logit, "decay_channel_offset": decay_channel_offset, "extra_log_decay": extra_log_decay, "removal_dependent_logit": removal_dependent_logit, "removal_channel_offset": removal_channel_offset, "head_norm_gain": head_norm_gain, "output_matrix": output_matrix, "expert_norm_gain": expert_norm_gain, "token_expert_index": token_expert_index, "token_expert_weight": token_expert_weight, "expert_gate_weight": expert_gate_weight, "expert_up_weight": expert_up_weight, "expert_down_weight": expert_down_weight}


group_epsilon = 0.00064
norm_epsilon = 1e-06
unit_epsilon = 1e-06
highest = lax.Precision.HIGHEST

def log_decay_series(decay_dependent_logit, decay_channel_offset, extra_log_decay):
    current_tier = decay_channel_offset[None, :] + decay_dependent_logit.astype(jnp.float32)
    return -jnp.exp(-jax.nn.softplus(-current_tier) - 0.5) + extra_log_decay

def learn_rates(removal_dependent_logit, removal_channel_offset):
    return jax.nn.sigmoid(removal_channel_offset[None, :] + removal_dependent_logit.astype(jnp.float32))

def unit_rows(key_heads):
    return key_heads * lax.rsqrt(lax.optimization_barrier(jnp.sum(key_heads * key_heads, axis=-1, keepdims=True)) + unit_epsilon)

def group_norm(heads_out, head_norm_gain):
    center = heads_out - lax.optimization_barrier(jnp.mean(heads_out, axis=-1, keepdims=True))
    spread = lax.optimization_barrier(jnp.mean(center * center, axis=-1, keepdims=True))
    scaled = center * lax.rsqrt(spread + group_epsilon)
    return (scaled.reshape(scaled.shape[0], -1) * head_norm_gain[None, :]).astype(jnp.bfloat16)

def split_heads(array):
    return array.astype(jnp.float32).reshape(array.shape[0], HEADS, HEAD)

def recurrence(receptance, key_matrix, values, log_decay_value, rates):
    read_heads = split_heads(receptance)
    key_heads = split_heads(key_matrix)
    value_heads = split_heads(values)
    decay_heads = jnp.exp(split_heads(log_decay_value))
    rate_heads = split_heads(rates)
    unit_heads = unit_rows(key_heads)

    def advance(memory, inputs):
        read_now, decay_now, key_now, value_now, unit_now, rate_now = inputs
        removed = jnp.einsum('hvk,hk->hv', memory, unit_now, precision=highest)
        memory = memory * decay_now[:, None, :] - removed[:, :, None] * (unit_now * rate_now)[:, None, :] + value_now[:, :, None] * key_now[:, None, :]
        return (memory, jnp.einsum('hvk,hk->hv', memory, read_now, precision=highest))
    initial = jnp.zeros((HEADS, HEAD, HEAD), jnp.float32)
    _, outputs = lax.scan(advance, initial, (read_heads, decay_heads, key_heads, value_heads, unit_heads, rate_heads))
    return outputs

def reference(residual, receptance, key_matrix, values, decay_dependent_logit, decay_channel_offset, extra_log_decay, removal_dependent_logit, removal_channel_offset, head_norm_gain, output_matrix, expert_norm_gain, token_expert_index, token_expert_weight, expert_gate_weight, expert_up_weight, expert_down_weight):
    log_decay_value = log_decay_series(decay_dependent_logit, decay_channel_offset, extra_log_decay)
    rates = learn_rates(removal_dependent_logit, removal_channel_offset)
    heads_out = recurrence(receptance, key_matrix, values, log_decay_value, rates)
    mixed = group_norm(heads_out, head_norm_gain)
    after_mix = residual.astype(jnp.float32) + jnp.dot(mixed, output_matrix, preferred_element_type=jnp.float32)
    normed = (after_mix * lax.rsqrt(lax.optimization_barrier(jnp.mean(after_mix * after_mix, axis=-1, keepdims=True)) + norm_epsilon) * expert_norm_gain[None, :]).astype(jnp.bfloat16)
    devices = N_SP * N_TP
    rows_dev = TOKENS // devices
    flat_ids = token_expert_index.reshape(devices, rows_dev * TOP)
    onehot = (flat_ids[:, :, None] == jnp.arange(EXPERTS, dtype=jnp.int32)[None, None, :]).astype(jnp.int32)
    slot_rank = lax.optimization_barrier(jnp.sum((jnp.cumsum(onehot, axis=1) - onehot) * onehot, axis=-1))
    per_expert = devices * CAP
    slot_index = (flat_ids * per_expert + jnp.arange(devices, dtype=jnp.int32)[:, None] * CAP + slot_rank).reshape(-1)
    token_index = jnp.arange(TOKENS * TOP, dtype=jnp.int32) // TOP
    row_table = jnp.full((EXPERTS * per_expert,), TOKENS, jnp.int32).at[slot_index].set(token_index)
    padded = jnp.concatenate([normed, jnp.zeros((1, D), jnp.bfloat16)], axis=0)
    group_width = FF // N_TP

    def run_expert(operands):
        row_ids, gate_weight, up_weight, down_weight = operands
        routed = padded[row_ids]
        gate_out = jnp.dot(routed, gate_weight, preferred_element_type=jnp.float32)
        up_out = jnp.dot(routed, up_weight, preferred_element_type=jnp.float32)
        hidden = (jax.nn.silu(gate_out) * up_out).astype(jnp.bfloat16)
        summed = jnp.zeros((routed.shape[0], D), jnp.float32)
        for quarter in range(N_TP):
            partial_sum = jnp.dot(hidden[:, quarter * group_width:(quarter + 1) * group_width], down_weight[quarter * group_width:(quarter + 1) * group_width], preferred_element_type=jnp.float32).astype(jnp.bfloat16)
            summed = summed + lax.optimization_barrier(partial_sum).astype(jnp.float32)
        return summed.astype(jnp.bfloat16)
    returned = lax.map(run_expert, (row_table.reshape(EXPERTS, per_expert), expert_gate_weight, expert_up_weight, expert_down_weight))
    picked = returned.reshape(EXPERTS * per_expert, D)[slot_index].reshape(TOKENS, TOP, D)
    routed_sum = lax.optimization_barrier(jnp.sum(token_expert_weight[:, :, None] * picked.astype(jnp.float32), axis=1))
    return (after_mix + routed_sum).astype(jnp.bfloat16)
```

```python
import functools

import jax
import jax.numpy as jnp
from jax import lax
from jax.experimental import pallas as pl
from jax.experimental.pallas import tpu as pltpu
from jax.sharding import Mesh
from jax.sharding import PartitionSpec as P

HEAD = 64
BLOCK = 64
SP = ("sp_0", "sp_1", "sp_2")
SP_TP = ("sp_0", "sp_1", "sp_2", "tp")
MESH_ID = pl.DeviceIdType.MESH

group_epsilon = 0.00064
norm_epsilon = 1e-06
unit_epsilon = 1e-06
bf16 = jnp.bfloat16
f32 = jnp.float32

NN = (((1,), (0,)), ((), ()))
NT = (((1,), (1,)), ((), ()))


def mm(a, b, dims=NN):
    return lax.dot_general(a, b, dims, preferred_element_type=f32)


def split(x):
    hi = x.astype(bf16)
    return hi, (x - hi.astype(f32)).astype(bf16)


def mm3(a, b, dims=NN):
    (ah, al), (bh, bl) = a, b
    return mm(ah, bh, dims) + (mm(ah, bl, dims) + mm(al, bh, dims))


def mm2(a, b, dims=NN):
    ah, al = a
    return mm(ah, b, dims) + mm(al, b, dims)


def local_kernel(
    rec_ref, key_ref, val_ref, ddl_ref, dco_ref, eld_ref, rdl_ref, rco_ref, rl_ref, pair_ref
):
    tokens, columns = rec_ref.shape
    heads = columns // HEAD
    blocks = tokens // BLOCK
    row = lax.broadcasted_iota(jnp.int32, (tokens, tokens), 0)
    col = lax.broadcasted_iota(jnp.int32, (tokens, tokens), 1)
    same = (row // BLOCK) == (col // BLOCK)
    lower = same & (row >= col)
    strict = same & (row > col)
    early = same & ((col % BLOCK) < BLOCK // 2)
    lower_one = lower.astype(f32)
    early_one = early.astype(f32)
    sums = jnp.concatenate(
        [lower_one - early_one, early_one, same.astype(f32) - early_one], axis=0
    ).astype(bf16)

    tier = dco_ref[...] + ddl_ref[...].astype(f32)
    log_decay = -0.6065306597126334 * jax.nn.sigmoid(tier) + eld_ref[...]
    rate = jax.nn.sigmoid(rco_ref[...] + rdl_ref[...].astype(f32))
    ld_hi, ld_rest = log_decay.astype(bf16), log_decay - log_decay.astype(bf16).astype(f32)
    ld_mid, ld_lo = split(ld_rest)
    summed = mm(sums, ld_hi) + (mm(sums, ld_mid) + mm(sums, ld_lo))
    rel, mid, late = summed[:tokens], summed[tokens : 2 * tokens], summed[2 * tokens :]
    up, down, up_before = jnp.exp(rel), jnp.exp(-rel), jnp.exp(rel - log_decay)
    from_start, to_end = jnp.exp(mid), jnp.exp(late)
    totals = jnp.exp(mid + late)
    read = rec_ref[...].astype(f32)
    keys = key_ref[...].astype(f32)
    vals = val_ref[...].astype(f32)
    read_all = read * up
    keyd_all = keys * down
    row_h = lax.broadcasted_iota(jnp.int32, (tokens, 2 * HEAD), 0)
    col_h = lax.broadcasted_iota(jnp.int32, (tokens, 2 * HEAD), 1)
    diagonal = col_h == (row_h % BLOCK)
    unit_one = (lax.broadcasted_iota(jnp.int32, (HEAD, 2 * HEAD), 0)
                == lax.broadcasted_iota(jnp.int32, (HEAD, 2 * HEAD), 1)).astype(f32)
    zeros = jnp.zeros((tokens, HEAD), f32)
    eye = (row == col).astype(f32)

    def wide(x):
        return jnp.concatenate([x, zeros], axis=1)

    per_head = []
    for h in range(heads):
        part = slice(h * HEAD, (h + 1) * HEAD)
        key_h = keys[:, part]
        unit = key_h * lax.rsqrt(jnp.sum(key_h * key_h, axis=-1, keepdims=True) + unit_epsilon)
        remove = -unit * up_before[:, part]
        write = unit * rate[:, part] * down[:, part]
        reads, keyd = read_all[:, part], keyd_all[:, part]
        rows2 = split(jnp.concatenate([remove, reads], axis=0))
        cols2 = split(jnp.concatenate([write, keyd], axis=0))
        grid = mm3(rows2, cols2, NT)
        couple_write = jnp.where(strict, grid[:tokens, :tokens], 0.0)
        couple_key = jnp.where(strict, grid[:tokens, tokens:], 0.0)
        read_write = jnp.where(lower, grid[tokens:, :tokens], 0.0)
        read_key = jnp.where(lower, grid[tokens:, tokens:], 0.0)
        per_head.append((remove, write, reads, keyd, couple_write, couple_key, read_write, read_key))

    inverses = []
    size = 1
    pair_mask = ((row // 2) == (col // 2)) & (row > col)
    for h in range(heads):
        inverses.append(eye + jnp.where(pair_mask, per_head[h][4], 0.0))
    size = 2
    while size < BLOCK:
        mask = ((row // (2 * size)) == (col // (2 * size))) & ((row // size) > (col // size))
        for h in range(heads):
            x = inverses[h]
            xs = split(x)
            inner = mm3(xs, split(jnp.where(mask, per_head[h][4], 0.0)))
            inverses[h] = x + mm3(split(inner), xs)
        size *= 2

    block_row = lax.broadcasted_iota(jnp.int32, (blocks * HEAD, tokens), 0) // HEAD
    block_col = lax.broadcasted_iota(jnp.int32, (blocks * HEAD, tokens), 1) // BLOCK
    block_mask = block_row == block_col
    for h in range(heads):
        part = slice(h * HEAD, (h + 1) * HEAD)
        remove, write, reads, keyd, couple_write, couple_key, read_write, read_key = per_head[h]
        start_h, end_h = from_start[:, part], to_end[:, part]
        value_w = jnp.concatenate([zeros, vals[:, part]], axis=1).astype(bf16)
        right = wide(remove * start_h) + mm2(split(couple_key), value_w)
        solved = mm3(split(inverses[h]), split(right))
        solved_s = split(solved)
        read_out = (
            wide(reads * start_h) + mm3(split(read_write), solved_s) + mm2(split(read_key), value_w)
        )
        ends = jnp.concatenate([write * end_h, keyd * end_h], axis=1).T
        end_write = jnp.where(block_mask, jnp.concatenate([ends[:HEAD]] * blocks, axis=0), 0.0)
        end_key = jnp.where(block_mask, jnp.concatenate([ends[HEAD:]] * blocks, axis=0), 0.0)
        pairs = (
            mm3(split(end_write), solved_s)
            + mm2(split(end_key), value_w)
            + jnp.where(diagonal, wide(totals[:, part]), 0.0)
        )
        before = [unit_one]
        for b in range(blocks):
            now = pairs[b * HEAD : (b + 1) * HEAD]
            if b == 0:
                before.append(now)
            else:
                offset = jnp.where(col_h[:HEAD] >= HEAD, now, 0.0)
                before.append(mm3(split(now[:, :HEAD]), split(before[-1])) + offset)
        pair_ref[h] = before[blocks]
        stacked = jnp.concatenate(before[:blocks], axis=0)
        readout = jnp.concatenate([read_out[:, :HEAD]] * blocks, axis=1)
        readout = jnp.where(block_mask.T if False else (row // BLOCK) == (col // HEAD), readout, 0.0)
        rl_ref[h] = mm3(split(readout), split(stacked)) + jnp.where(col_h >= HEAD, read_out, 0.0)


def local_terms(rec, key, val, ddl, dco, eld, rdl, rco):
    heads = rec.shape[1] // HEAD
    vmem = pl.BlockSpec(memory_space=pltpu.VMEM)
    return pl.pallas_call(
        local_kernel,
        out_shape=(
            jax.ShapeDtypeStruct((heads, rec.shape[0], 2 * HEAD), f32),
            jax.ShapeDtypeStruct((heads, HEAD, 2 * HEAD), f32),
        ),
        in_specs=[vmem] * 8,
        out_specs=(vmem, vmem),
        name="local_terms",
    )(rec, key, val, ddl, dco.reshape(1, -1), eld, rdl, rco.reshape(1, -1))


def compose(first, second):
    col = lax.broadcasted_iota(jnp.int32, (HEAD, 2 * HEAD), 1)
    out = []
    for a, b in zip(first, second):
        out.append(mm3(split(b[:, :HEAD]), split(a)) + jnp.where(col >= HEAD, b, 0.0))
    return out


def choose(which, options):
    out = options[0]
    for k in range(1, len(options)):
        out = [jnp.where(which == k, b, a) for a, b in zip(out, options[k])]
    return out


def prefix_kernel(
    rl_ref, pair_ref, gain_ref, mixed_ref,
    own_buf, core_buf, chip_buf, y_buf, plane_buf, z_buf, send_buf, x_buf, send_sem, recv_sem, copy_sem,
):
    heads = pair_ref.shape[0]
    z, y, c, x = (lax.axis_index(a) for a in ("sp_0", "sp_1", "sp_2", "tp"))
    peers = [{"sp_2": 1 - c}]
    for axis, at in (("sp_1", y), ("sp_0", z), ("tp", x)):
        peers += [{axis: lax.rem(at + k, 4)} for k in (1, 2, 3)]
    barrier = pltpu.get_barrier_semaphore()
    for peer in peers:
        pl.semaphore_signal(barrier, inc=1, device_id=peer, device_id_type=MESH_ID)
    pl.semaphore_wait(barrier, len(peers))

    def remote(src, dst, n, peer):
        return pltpu.make_async_remote_copy(
            src_ref=src, dst_ref=dst, send_sem=send_sem.at[n], recv_sem=recv_sem.at[n],
            device_id=peer, device_id_type=MESH_ID,
        )

    unit_one = (lax.broadcasted_iota(jnp.int32, (HEAD, 2 * HEAD), 0)
                == lax.broadcasted_iota(jnp.int32, (HEAD, 2 * HEAD), 1)).astype(f32)
    nothing = [unit_one] * heads

    own = [pair_ref[h] for h in range(heads)]
    for h in range(heads):
        own_buf[h] = own[h].astype(bf16)
    to_core = remote(own_buf, core_buf, 0, peers[0])
    to_core.start()
    to_core.wait_recv()
    other = [core_buf[h].astype(f32) for h in range(heads)]
    first = choose(c, [own, other])
    second = choose(c, [other, own])
    chip = compose(first, second)
    in_core = choose(c, [nothing, other])

    for h in range(heads):
        chip_buf[h] = chip[h].astype(bf16)
    sends = []
    for k in (1, 2, 3):
        sends.append(remote(chip_buf, y_buf.at[k - 1], k, peers[k]))
    for s in sends:
        s.start()
    for s in sends:
        s.wait_recv()
    slots = [[y_buf[k, h].astype(f32) for h in range(heads)] for k in range(3)]
    ys = []
    for j in range(4):
        ys.append(choose(lax.rem(y - j + 4, 4), [chip] + slots))
    y01 = compose(ys[0], ys[1])
    y23 = compose(ys[2], ys[3])
    plane = compose(y01, y23)
    for h in range(heads):
        plane_buf[h] = plane[h].astype(bf16)
    zsends = []
    for k in (1, 2, 3):
        zsends.append(remote(plane_buf, z_buf.at[k - 1], 3 + k, peers[3 + k]))
    for s in zsends:
        s.start()
    y012 = compose(y01, ys[2])
    in_plane = compose(choose(y, [nothing, ys[0], y01, y012]), in_core)
    for s in zsends:
        s.wait_recv()
    zslots = [[z_buf[k, h].astype(f32) for h in range(heads)] for k in range(3)]
    zs = []
    for j in range(3):
        zs.append(choose(lax.rem(z - j + 4, 4), [plane] + zslots))
    z01 = compose(zs[0], zs[1])
    z012 = compose(z01, zs[2])
    whole = compose(choose(z, [nothing, zs[0], z01, z012]), in_plane)

    mixed = []
    for h in range(heads):
        rl = rl_ref[h]
        out = (mm3(split(rl[:, :HEAD]), split(whole[h])) + rl)[:, HEAD:]
        center = out - jnp.mean(out, axis=-1, keepdims=True)
        spread = jnp.mean(center * center, axis=-1, keepdims=True)
        mixed.append(center * lax.rsqrt(spread + group_epsilon))
    mixed = (jnp.concatenate(mixed, axis=1) * gain_ref[...]).astype(bf16)
    rows = mixed.shape[0] // 4
    send_buf[...] = mixed.reshape(4, rows, mixed.shape[1])
    xsends = []
    for k in (1, 2, 3):
        to = lax.rem(x + k, 4)
        xsends.append(remote(send_buf.at[to], x_buf.at[k - 1], 6 + k, {"tp": to}))
    for s in xsends:
        s.start()
    mixed_ref[x] = send_buf[x]
    for k in (1, 2, 3):
        xsends[k - 1].wait_recv()
        mixed_ref[lax.rem(x - k + 4, 4)] = x_buf[k - 1]
    for s in [to_core] + sends + zsends + xsends:
        s.wait_send()


def prefix_and_norm(rl, pair, gain):
    heads, tokens, _ = rl.shape
    vmem = pl.BlockSpec(memory_space=pltpu.VMEM)
    one = pltpu.VMEM((heads, HEAD, 2 * HEAD), bf16)
    three = pltpu.VMEM((3, heads, HEAD, 2 * HEAD), bf16)
    return pl.pallas_call(
        prefix_kernel,
        out_shape=jax.ShapeDtypeStruct((4, tokens // 4, heads * HEAD), bf16),
        in_specs=[vmem] * 3,
        out_specs=vmem,
        scratch_shapes=[
            one, one, one, three, one, three,
            pltpu.VMEM((4, tokens // 4, heads * HEAD), bf16),
            pltpu.VMEM((3, tokens // 4, heads * HEAD), bf16),
            pltpu.SemaphoreType.DMA((10,)),
            pltpu.SemaphoreType.DMA((10,)),
            pltpu.SemaphoreType.DMA,
        ],
        compiler_params=pltpu.CompilerParams(collective_id=0, has_side_effects=True),
        name="prefix_and_norm",
    )(rl, pair, gain.reshape(1, -1))


def cut_along(x, dim, devices):
    before, after = (x.shape[:dim], x.shape[dim + 1 :])
    return jnp.moveaxis(x.reshape(*before, devices, -1, *after), dim, 0)


def summed_on_arrival(x, axis, dim):
    devices = lax.axis_size(axis)
    parts = lax.all_to_all(cut_along(x, dim, devices), axis, 0, 0, tiled=True)
    return jnp.sum(parts.astype(jnp.float32), axis=0)


def expert_hidden(routed, gate_weight, up_weight):
    gate_out = jnp.dot(routed, gate_weight, preferred_element_type=jnp.float32)
    up_out = jnp.dot(routed, up_weight, preferred_element_type=jnp.float32)
    return (jax.nn.silu(gate_out) * up_out).astype(jnp.bfloat16)


def body(
    residual,
    receptance,
    key_matrix,
    values,
    decay_dependent_logit,
    decay_channel_offset,
    extra_log_decay,
    removal_dependent_logit,
    removal_channel_offset,
    head_norm_gain,
    output_matrix,
    expert_norm_gain,
    token_expert_index,
    token_expert_weight,
    expert_gate_weight,
    expert_up_weight,
    expert_down_weight,
):
    rl, pair = local_terms(
        receptance, key_matrix, values, decay_dependent_logit, decay_channel_offset,
        extra_log_decay, removal_dependent_logit, removal_channel_offset,
    )
    mixed = prefix_and_norm(rl, pair, head_norm_gain)
    mixed_tokens = mixed.transpose(1, 0, 2).reshape(mixed.shape[1], -1)
    after_mix = residual.astype(jnp.float32) + jnp.dot(
        mixed_tokens, output_matrix, preferred_element_type=jnp.float32
    )
    normed = (
        after_mix
        * lax.rsqrt(jnp.mean(after_mix * after_mix, axis=-1, keepdims=True) + norm_epsilon)
        * expert_norm_gain[None, :]
    ).astype(jnp.bfloat16)
    rows_dev, width = normed.shape
    top_count = token_expert_index.shape[1]
    experts = lax.axis_size(SP)
    group_size = lax.axis_size("tp")
    cap = 2 * rows_dev * top_count // experts
    flat_ids = token_expert_index.reshape(-1)
    onehot = (flat_ids[:, None] == jnp.arange(experts, dtype=jnp.int32)[None, :]).astype(jnp.int32)
    slot_rank = jnp.sum((jnp.cumsum(onehot, axis=0) - onehot) * onehot, axis=1)
    slot_index = flat_ids * cap + slot_rank
    token_index = jnp.arange(rows_dev * top_count, dtype=jnp.int32) // top_count
    outgoing = (
        jnp.zeros((experts * cap, width), jnp.bfloat16).at[slot_index].set(normed[token_index])
    )
    copies = jnp.broadcast_to(
        outgoing.reshape(experts, 1, cap, width), (experts, group_size, cap, width)
    )
    arrived = lax.all_to_all(
        copies.reshape(experts * group_size, cap, width),
        SP_TP,
        split_axis=0,
        concat_axis=0,
        tiled=True,
    )
    hidden = expert_hidden(arrived.reshape(-1, width), expert_gate_weight[0], expert_up_weight[0])
    hidden = (
        hidden.reshape(experts, group_size, cap, -1)
        .transpose(1, 0, 2, 3)
        .reshape(experts * group_size * cap, -1)
    )
    summed = summed_on_arrival(
        jnp.dot(hidden, expert_down_weight[0], preferred_element_type=jnp.float32).astype(
            jnp.bfloat16
        ),
        "tp",
        0,
    )
    returned = lax.all_to_all(
        summed.astype(jnp.bfloat16).reshape(experts, cap, width),
        SP,
        split_axis=0,
        concat_axis=0,
        tiled=True,
    )
    picked = returned.reshape(experts * cap, width)[slot_index].reshape(rows_dev, top_count, width)
    routed_sum = jnp.sum(token_expert_weight[:, :, None] * picked.astype(jnp.float32), axis=1)
    return (after_mix + routed_sum).astype(jnp.bfloat16)


def solution(mesh):
    split = Mesh(mesh.devices.reshape(4, 4, 2, mesh.shape["tp"]), ("sp_0", "sp_1", "sp_2", "tp"))
    placed = (
        P(SP_TP, None),
        P(SP, "tp"),
        P(SP, "tp"),
        P(SP, "tp"),
        P(SP, "tp"),
        P("tp"),
        P(SP, "tp"),
        P(SP, "tp"),
        P("tp"),
        P("tp"),
        P(),
        P(),
        P(SP_TP, None),
        P(SP_TP, None),
        P(SP, None, "tp"),
        P(SP, None, "tp"),
        P(SP, "tp", None),
    )
    return jax.shard_map(
        body, mesh=split, in_specs=placed, out_specs=P(SP_TP, None), check_vma=False
    )
```
